256 devices in a mesh: grp: 2 (over z), ep: 16 (over y, core), tp: 8 (over x).
Axes of the slice: x: 8, y: 8, z: 2, core: 2. Of those that a mesh axis runs over, the one named last changes fastest.
The devices are a block of a 8x8x16 slice.
Arguments:
- mixer_in: bfloat16 [32768, 2048], P(('grp', 'ep', 'tp')), parts along dimension 0, may hold values from -600 to 600
- mixer_gain: float32 [2048], replicated, may hold values from 0.1 to 1.9
- w_query: bfloat16 [2048, 1024], P(None, 'tp'), may hold values from -6 to 6
- w_key: bfloat16 [2048, 512], P(None, 'tp'), may hold values from -0.1875 to 0.1875
- w_value: bfloat16 [2048, 512], P(None, 'tp'), may hold values from -0.25 to 0.25
- sink_logit: float32 [16], P('tp'), may hold values from 3 to 9
- moe_in: bfloat16 [32768, 2048], P(('grp', 'ep', 'tp')), parts along dimension 0, may hold values from -600 to 600
- moe_gain: float32 [2048], replicated, may hold values from 0.1 to 1.9
- router: bfloat16 [2048, 128], replicated, may hold values from -0.25 to 0.25
- routes: int32 [32768, 4], P(('grp', 'ep', 'tp')), parts along dimension 0, may hold values from 0 to 127, all different within a row; in each aligned block of 128 rows (0 to 127, 128 to 255, ...) at most 6 rows name the same one
- expert_gate: bfloat16 [128, 2048, 512], P(('ep', 'tp')), may hold values from -0.125 to 0.125
- expert_up: bfloat16 [128, 2048, 512], P(('ep', 'tp')), may hold values from -0.125 to 0.125
- expert_down: bfloat16 [128, 512, 2048], P(('ep', 'tp')), may hold values from -0.25 to 0.25
- shared_gate: bfloat16 [2048, 512], P(None, 'tp'), may hold values from -0.125 to 0.125
- shared_up: bfloat16 [2048, 512], P(None, 'tp'), may hold values from -0.125 to 0.125
- shared_down: bfloat16 [512, 2048], P('tp'), may hold values from -0.25 to 0.25
Outputs:
- mixed: bfloat16 [32768, 1024], P(('grp', 'ep'), 'tp'), parts along dimension 0
- moe_out: bfloat16 [32768, 2048], P(('grp', 'ep', 'tp')), parts along dimension 0
The draws below stay inside these ranges and needn't reach their ends.
There are 2 independent parts, one for each index of `grp`. The reference program is written for one: setup_inputs(seed, part) draws one part's arguments, and reference() takes and returns one part's arrays. A program takes and returns all parts, laid end to end along the dimension named above; an argument that names none is the same for every part. Nothing has to cross between parts.
Inputs may be any that keep to these rules, and one draw needn't show every extreme that they name: `routes`: each row names 4 different experts. Within the rows of one device (aligned blocks of 128 rows) no expert is named by more than 6 rows, a bound that some block reaches.
All inputs are finite; a program needn't handle non-finite values.
Results may differ from the reference program's by a relative error of at most 0.012.
Values may be sent and summed in bfloat16 or wider, within the bound.
No kernel may reach another device: no remote copies, remote signals or barrier semaphores. Data moves between devices by JAX's collectives and lax.ppermute only.
A program may use at most 128 MiB of HBM per device.

```python
import math
import jax
import jax.numpy as jnp
import numpy as np
from jax import lax

D = 2048
HEADS = 16
KV_HEADS = 8
HEAD_DIM = 64
WINDOW = 128
EFF = 512
SFF = 512
TOP_K = 4
ROWS = 128
TOKENS = 16384
EXPERTS = 128
CAP = 6


def draw_mixer_in(key, part):
    values = jnp.clip(jax.random.normal(jax.random.fold_in(key, 1), (TOKENS, D), jnp.float32), -6.0, 6.0)
    return values.astype(jnp.bfloat16)


def draw_moe_in(key, part):
    values = jnp.clip(jax.random.normal(jax.random.fold_in(key, 4), (TOKENS, D), jnp.float32), -6.0, 6.0)
    return values.astype(jnp.bfloat16)


def attention_weights(key):
    key_part, query_part = jax.random.split(jax.random.fold_in(key, 7), 2)
    spread = (2.0 / D) ** 0.5
    keys_weight = jnp.clip(jax.random.normal(key_part, (D, KV_HEADS, HEAD_DIM), jnp.float32), -6.0, 6.0) * spread
    query_weight = jnp.clip(jax.random.normal(query_part, (D, HEADS, HEAD_DIM), jnp.float32), -6.0, 6.0) * spread
    return (query_weight.reshape(D, HEADS * HEAD_DIM), keys_weight.reshape(D, KV_HEADS * HEAD_DIM))


def draw_w_query(key, part):
    return attention_weights(key)[0].astype(jnp.bfloat16)


def draw_w_key(key, part):
    return attention_weights(key)[1].astype(jnp.bfloat16)


def shard_levels(key, extent, pieces, low, high):
    gain, own = 1.0, jax.random.fold_in(key, 6)
    for axis_at, parts in pieces:
        steps = jnp.exp(jax.random.uniform(jax.random.fold_in(own, axis_at), (parts,), jnp.float32, low / len(pieces), high / len(pieces)))
        gain = gain * jnp.repeat(steps, extent[axis_at] // parts).reshape([-1 if axis == axis_at else 1 for axis in range(len(extent))])
    return gain


def shared_out(stream_key, own, number, rows, amount, top, bound, skew):
    order = jax.random.permutation(stream_key, amount)
    heavy_load, usual = shares(amount, rows * top, bound, skew, True), shares(amount, rows * top, bound, skew, False)
    places = jnp.arange(amount)

    def named(lengths, offset_by):
        used = int((lengths > 0).sum())
        fixed = max(1, used // 4)
        shifted = fixed + (places - fixed + offset_by * (used - fixed)) % max(1, amount - fixed)
        return jnp.zeros((amount,), jnp.int32).at[order[jnp.where(places < fixed, places, shifted)]].set(jnp.asarray(lengths, jnp.int32))

    lengths = jnp.where(number % 4 == 0, named(heavy_load, number // 4), named(usual, number - number // 4 - 1))
    mixed = jax.random.permutation(jax.random.fold_in(own, 3), amount)
    giver, taker = mixed[0:amount // 2 * 2:2], mixed[1:amount // 2 * 2:2]
    margin = jnp.minimum(lengths[giver] - 1, bound - lengths[taker]) // 2
    margin = jnp.where((giver == order[0]) | (taker == order[0]) | (lengths[taker] == 0), 0, jnp.maximum(margin, 0))
    shifted = jax.random.randint(jax.random.fold_in(own, 4), (amount // 2,), 0, 1 << 20) % (margin + 1)
    lengths = lengths.at[giver].add(-shifted).at[taker].add(shifted)
    members = jnp.searchsorted(jnp.cumsum(lengths), jnp.arange(rows * top), side="right").astype(jnp.int32)
    listing = members.reshape(top, rows).T
    listing = listing[jax.random.permutation(jax.random.fold_in(own, 1), rows)]
    offset_by = jax.random.randint(jax.random.fold_in(own, 2), (rows, 1), 0, top)
    return jnp.take_along_axis(listing, (jnp.arange(top)[None, :] + offset_by) % top, axis=1)


def shares(amount, total, bound, skew, full):
    weights = [(1 << 20) // math.isqrt(grade ** skew) + 1 for grade in range(1, amount + 1)]
    largest = bound if full else min(bound, max(-(-total // amount), total * weights[0] // sum(weights)))
    least = 1 if total - largest >= amount - 1 else 0
    given, surplus = [largest] + [least] * (amount - 1), total - largest - least * (amount - 1)
    while surplus > 0:
        movable = [i for i in range(1, amount) if given[i] < largest] or [i for i in range(1, amount) if given[i] < bound]
        pool, remaining = sum([weights[i] for i in movable]), surplus
        for i in movable:
            extra = min(bound - given[i], max(1, remaining * weights[i] // pool), surplus)
            given[i] = given[i] + extra
            surplus = surplus - extra
    return np.array(given)


def bell_draw(key, shape, scale, limit, cuts=(), kind=jnp.bfloat16):
    array = jax.random.normal(key, shape, jnp.float32) * scale
    if len(cuts) > 0:
        array = shard_levels(key, shape, cuts, -0.22, 0.18) * array
    return jnp.clip(array, min=-limit, max=limit).astype(kind)


def setup_inputs(seed: int = 0, part: int = 0) -> dict:
    key_list = jax.random.split(jax.random.key(seed), 17)
    own_keys = jax.random.split(jax.random.fold_in(key_list[16], part), 17)
    mixer_in = draw_mixer_in(jax.random.fold_in(jax.random.fold_in(key_list[16], part), 71), part)
    mixer_gain = jnp.clip(1.0 + 0.18 * jax.random.normal(key_list[1], (D,), jnp.float32), 0.1, 1.9)
    w_query = draw_w_query(jax.random.fold_in(key_list[16], 71), part)
    w_key = draw_w_key(jax.random.fold_in(key_list[16], 71), part)
    w_value = bell_draw(key_list[4], (D, KV_HEADS * HEAD_DIM), (D // 4) ** -0.5, 0.25, ((1, 8),))
    sink_logit = jnp.clip(3.0 + 6.0 * jax.random.uniform(key_list[5], (HEADS,), jnp.float32) ** shard_levels(key_list[5], (HEADS,), ((0, 8),), -0.2, 0.2), 3.0, 9.0)
    moe_in = draw_moe_in(jax.random.fold_in(jax.random.fold_in(key_list[16], part), 71), part)
    moe_gain = jnp.clip(1.0 + 0.18 * jax.random.normal(key_list[7], (D,), jnp.float32), 0.1, 1.9)
    router = bell_draw(key_list[8], (D, EXPERTS), (D // 4) ** -0.5, 0.25)
    routes_keys = jax.random.split(jax.random.fold_in(own_keys[9], 1), TOKENS // ROWS)
    routes_turns = jax.random.permutation(jax.random.fold_in(own_keys[9], 3), TOKENS // ROWS)
    routes = jax.vmap(lambda own, number: shared_out(jax.random.fold_in(own_keys[9], 2), own, number, ROWS, EXPERTS, TOP_K, CAP, 2))(routes_keys, routes_turns).reshape((TOKENS, TOP_K))
    expert_gate = bell_draw(key_list[10], (EXPERTS, D, EFF), D ** -0.5, 0.125, ((0, 128),))
    expert_up = bell_draw(key_list[11], (EXPERTS, D, EFF), D ** -0.5, 0.125, ((0, 128),))
    expert_down = bell_draw(key_list[12], (EXPERTS, EFF, D), EFF ** -0.5, 0.25, ((0, 128),))
    shared_gate = bell_draw(key_list[13], (D, SFF), D ** -0.5, 0.125, ((1, 8),))
    shared_up = bell_draw(key_list[14], (D, SFF), D ** -0.5, 0.125, ((1, 8),))
    shared_down = bell_draw(key_list[15], (SFF, D), SFF ** -0.5, 0.25, ((0, 8),))
    return dict(mixer_in=mixer_in, mixer_gain=mixer_gain, w_query=w_query, w_key=w_key, w_value=w_value, sink_logit=sink_logit, moe_in=moe_in, moe_gain=moe_gain, router=router, routes=routes, expert_gate=expert_gate, expert_up=expert_up, expert_down=expert_down, shared_gate=shared_gate, shared_up=shared_up, shared_down=shared_down)


EPS = 1e-06
THETA = 10000.0
ROUTED_SCALE = 2.5

def rms_rows(row_block, gain_vector):
    values = row_block.astype(jnp.float32)
    factor = lax.rsqrt(lax.optimization_barrier(jnp.mean(values * values, axis=-1, keepdims=True)) + EPS)
    return (values * factor * gain_vector.astype(jnp.float32)).astype(jnp.bfloat16)

def rotate(head_rows, positions):
    half_width = head_rows.shape[-1] // 2
    inverse = THETA ** (-(jnp.arange(half_width, dtype=jnp.float32) * 2.0) / head_rows.shape[-1])
    angles = positions.astype(jnp.float32)[:, None] * inverse[None, :]
    cosine_table = jnp.cos(angles)[:, None, :]
    sine_table = jnp.sin(angles)[:, None, :]
    first_half = head_rows[..., :half_width]
    second_half = head_rows[..., half_width:]
    return jnp.concatenate([first_half * cosine_table - second_half * sine_table, second_half * cosine_table + first_half * sine_table], axis=-1)

def window_attention(query_rows, key_rows, value_rows, sink_logit):
    length = query_rows.shape[0]
    head_count = query_rows.shape[1]
    kv_count = key_rows.shape[1]
    group_size = head_count // kv_count
    head_width = query_rows.shape[2]
    block_rows = min(512, length)
    padding = ((WINDOW, WINDOW), (0, 0), (0, 0))
    key_table = jnp.pad(key_rows, padding)
    value_table = jnp.pad(value_rows, padding)
    grouped = query_rows.reshape(length, kv_count, group_size, head_width)
    row_ids = jnp.arange(block_rows, dtype=jnp.int32)[:, None]
    col_ids = jnp.arange(block_rows + 2 * WINDOW, dtype=jnp.int32)[None, :]
    sink_table = sink_logit.astype(jnp.float32).reshape(kv_count, group_size)[:, :, None, None]

    def one_block(block_index):
        block_start = block_index * block_rows
        query_block = lax.dynamic_slice_in_dim(grouped, block_start, block_rows, 0).astype(jnp.float32)
        key_block = lax.dynamic_slice_in_dim(key_table, block_start, block_rows + 2 * WINDOW, 0).astype(jnp.float32)
        value_block = lax.dynamic_slice_in_dim(value_table, block_start, block_rows + 2 * WINDOW, 0).astype(jnp.float32)
        scores = jnp.einsum('qkgd,ckd->kgqc', query_block, key_block) * head_width ** (-0.5)
        key_pos = block_start - WINDOW + col_ids
        query_pos = block_start + row_ids
        in_window = (jnp.abs(key_pos - query_pos) <= WINDOW) & (key_pos >= 0) & (key_pos < length)
        scores = jnp.where(in_window[None, None], scores, -jnp.inf)
        row_max = jnp.maximum(lax.optimization_barrier(jnp.max(scores, axis=-1, keepdims=True)), sink_table)
        weights = jnp.exp(scores - row_max)
        denominator = lax.optimization_barrier(jnp.sum(weights, axis=-1, keepdims=True)) + jnp.exp(sink_table - row_max)
        probability = (weights / denominator).astype(jnp.bfloat16)
        output = jnp.einsum('kgqc,ckd->qkgd', probability.astype(jnp.float32), value_block)
        return output.reshape(block_rows, head_count * head_width).astype(jnp.bfloat16)
    blocks_out = lax.map(one_block, jnp.arange(length // block_rows, dtype=jnp.int32))
    return blocks_out.reshape(length, head_count * head_width)

def reference(mixer_in, mixer_gain, w_query, w_key, w_value, sink_logit, moe_in, moe_gain, router, routes, expert_gate, expert_up, expert_down, shared_gate, shared_up, shared_down):
    normed_first = rms_rows(mixer_in, mixer_gain)
    positions = jnp.arange(normed_first.shape[0], dtype=jnp.int32)
    query_rows = rotate(jnp.dot(normed_first, w_query, preferred_element_type=jnp.float32).reshape(-1, HEADS, HEAD_DIM), positions).astype(jnp.bfloat16)
    key_rows = rotate(jnp.dot(normed_first, w_key, preferred_element_type=jnp.float32).reshape(-1, KV_HEADS, HEAD_DIM), positions).astype(jnp.bfloat16)
    value_rows = jnp.dot(normed_first, w_value, preferred_element_type=jnp.float32).astype(jnp.bfloat16)
    value_rows = value_rows.reshape(-1, KV_HEADS, HEAD_DIM)
    mixed = window_attention(query_rows, key_rows, value_rows, sink_logit)
    normed_second = rms_rows(moe_in, moe_gain)
    affinity = jax.nn.sigmoid(jnp.dot(normed_second, router, preferred_element_type=jnp.float32))
    chosen = jnp.take_along_axis(affinity, routes, axis=1)
    route_weight = ROUTED_SCALE * chosen / lax.optimization_barrier(jnp.sum(chosen, axis=-1, keepdims=True))
    shared_hidden = (jax.nn.silu(jnp.dot(normed_second, shared_gate, preferred_element_type=jnp.float32)) * jnp.dot(normed_second, shared_up, preferred_element_type=jnp.float32)).astype(jnp.bfloat16)
    shared = jnp.dot(shared_hidden, shared_down, preferred_element_type=jnp.float32)
    token_count = routes.shape[0]
    sources = token_count // ROWS
    per_source = routes.reshape(sources, ROWS * TOP_K)
    one_hot = (per_source[:, :, None] == jnp.arange(EXPERTS, dtype=jnp.int32)[None, None, :]).astype(jnp.int32)
    slot_index = lax.optimization_barrier(jnp.sum((jnp.cumsum(one_hot, axis=1) - 1) * one_hot, axis=-1))
    source_ids = jnp.arange(sources, dtype=jnp.int32)[:, None]
    column = (source_ids * CAP + slot_index).reshape(-1).astype(jnp.int32)
    token_ids = jnp.arange(token_count * TOP_K, dtype=jnp.int32) // TOP_K
    flat_routes = routes.reshape(-1)
    row_table = jnp.full((EXPERTS, sources * CAP), token_count, jnp.int32).at[flat_routes, column].set(token_ids)
    weight_table = jnp.zeros((EXPERTS, sources * CAP), jnp.float32).at[flat_routes, column].set(route_weight.reshape(-1))
    padded_rows = jnp.concatenate([normed_second, jnp.zeros((1, normed_second.shape[1]), jnp.bfloat16)], axis=0)

    def one_expert(totals, inputs):
        row_ids, scales, gate_weight, up_weight, down_weight = inputs
        gathered = padded_rows[row_ids]
        hidden = (jax.nn.silu(jnp.dot(gathered, gate_weight, preferred_element_type=jnp.float32)) * jnp.dot(gathered, up_weight, preferred_element_type=jnp.float32)).astype(jnp.bfloat16)
        result = jnp.dot(hidden, down_weight, preferred_element_type=jnp.float32).astype(jnp.bfloat16)
        return (totals.at[row_ids].add(result.astype(jnp.float32) * scales[:, None]), None)
    totals, _ = lax.scan(one_expert, jnp.zeros((token_count + 1, normed_second.shape[1]), jnp.float32), (row_table, weight_table, expert_gate, expert_up, expert_down))
    moe_out = (totals[:token_count] + shared).astype(jnp.bfloat16)
    return (mixed, moe_out)
```

```python
import jax
import jax.numpy as jnp
from jax import lax
from jax.experimental import pallas as pl
from jax.experimental.pallas import tpu as pltpu
from jax.sharding import PartitionSpec as P

HEAD_DIM = 64
WINDOW = 128


EPS = 1e-06
THETA = 10000.0
ROUTED_SCALE = 2.5


def extended(block, sides, width):
    for axis, dim in sides:
        count = lax.axis_size(axis)
        forward = [(i, i + 1) for i in range(count - 1)]
        backward = [(target, source) for source, target in forward]
        low = lax.ppermute(
            lax.slice_in_dim(block, block.shape[dim] - width, None, axis=dim), axis, forward
        )
        high = lax.ppermute(lax.slice_in_dim(block, 0, width, axis=dim), axis, backward)
        block = jnp.concatenate([low, block, high], axis=dim)
    return block


def rms_rows(row_block, gain_vector):
    values = row_block.astype(jnp.float32)
    factor = lax.rsqrt(jnp.mean(values * values, axis=-1, keepdims=True) + EPS)
    return (values * factor * gain_vector).astype(jnp.bfloat16)


def rotate(head_rows, positions):
    half_width = head_rows.shape[-1] // 2
    inverse = THETA ** (-(jnp.arange(half_width, dtype=jnp.float32) * 2.0) / head_rows.shape[-1])
    angles = positions.astype(jnp.float32)[:, None] * inverse[None, :]
    cosine_table = jnp.cos(angles)[:, None, :]
    sine_table = jnp.sin(angles)[:, None, :]
    first_half = head_rows[..., :half_width]
    second_half = head_rows[..., half_width:]
    return jnp.concatenate(
        [
            first_half * cosine_table - second_half * sine_table,
            second_half * cosine_table + first_half * sine_table,
        ],
        axis=-1,
    )


def attend(query_rows, stacked, sink_logit, offset, seq_length):
    span_rows, head_count, head_width = query_rows.shape
    kv_local = stacked.shape[1] // (2 * head_width)
    group_size = head_count // kv_local
    key_table = stacked[:, : kv_local * head_width].reshape(-1, kv_local, head_width)
    value_table = stacked[:, kv_local * head_width :].reshape(-1, kv_local, head_width)
    block_rows = 512
    grouped = query_rows.reshape(span_rows, kv_local, group_size, head_width)
    row_ids = jnp.arange(block_rows, dtype=jnp.int32)[:, None]
    col_ids = jnp.arange(block_rows + 2 * WINDOW, dtype=jnp.int32)[None, :]
    sink_table = sink_logit.reshape(kv_local, group_size)[:, :, None, None]

    def one_block(block_index):
        block_start = block_index * block_rows
        query_block = lax.dynamic_slice_in_dim(grouped, block_start, block_rows, 0)
        key_block = lax.dynamic_slice_in_dim(key_table, block_start, block_rows + 2 * WINDOW, 0)
        value_block = lax.dynamic_slice_in_dim(value_table, block_start, block_rows + 2 * WINDOW, 0)
        scores = jnp.einsum(
            "qkgd,ckd->kgqc", query_block, key_block, preferred_element_type=jnp.float32
        ) * head_width ** (-0.5)
        key_pos = offset + block_start - WINDOW + col_ids
        query_pos = offset + block_start + row_ids
        in_window = (
            (jnp.abs(key_pos - query_pos) <= WINDOW) & (key_pos >= 0) & (key_pos < seq_length)
        )
        scores = jnp.where(in_window[None, None], scores, -jnp.inf)
        row_max = jnp.maximum(jnp.max(scores, axis=-1, keepdims=True), sink_table)
        weights = jnp.exp(scores - row_max)
        denominator = jnp.sum(weights, axis=-1, keepdims=True) + jnp.exp(sink_table - row_max)
        probability = (weights / denominator).astype(jnp.bfloat16)
        output = jnp.einsum(
            "kgqc,ckd->qkgd", probability, value_block, preferred_element_type=jnp.float32
        )
        return output.reshape(block_rows, head_count * head_width).astype(jnp.bfloat16)

    blocks_out = lax.map(one_block, jnp.arange(span_rows // block_rows, dtype=jnp.int32))
    return blocks_out.reshape(span_rows, head_count * head_width)


CAP = 6
FOLD = 4
TILE = CAP * FOLD


def reorder(cells, inverse):
    size = cells * TILE
    row = lax.broadcasted_iota(jnp.int32, (size, size), 1 if inverse else 0)
    col = lax.broadcasted_iota(jnp.int32, (size, size), 0 if inverse else 1)
    fold = row // (cells * CAP)
    within = row - fold * (cells * CAP)
    cell = within // CAP
    wanted = cell * TILE + fold * CAP + (within - cell * CAP)
    return (wanted == col).astype(jnp.bfloat16)


CELLS = 16


def expert_kernel(rows_ref, gate_ref, up_ref, down_ref, into_ref, outof_ref, out_ref):
    f32, bf16 = jnp.float32, jnp.bfloat16
    size = CELLS * TILE
    pieces = rows_ref.shape[0] // size
    quarter = rows_ref.shape[1]
    flat = []
    for piece in range(pieces):
        block = jnp.dot(
            into_ref[...], rows_ref[piece * size : (piece + 1) * size], preferred_element_type=f32
        ).astype(bf16)
        flat.append(
            jnp.concatenate(
                [block[f * CELLS * CAP : (f + 1) * CELLS * CAP] for f in range(FOLD)], axis=1
            )
        )
    tokens = jnp.concatenate(flat, axis=0)
    gate = jnp.dot(tokens, gate_ref[...], preferred_element_type=f32)
    up = jnp.dot(tokens, up_ref[...], preferred_element_type=f32)
    hidden = (gate * (1.0 / (1.0 + jnp.exp(-gate))) * up).astype(bf16)
    result = jnp.dot(hidden, down_ref[...], preferred_element_type=f32).astype(bf16)
    for piece in range(pieces):
        part = result[piece * CELLS * CAP : (piece + 1) * CELLS * CAP]
        block = jnp.concatenate(
            [part[:, f * quarter : (f + 1) * quarter] for f in range(FOLD)], axis=0
        )
        out_ref[piece * size : (piece + 1) * size] = jnp.dot(
            outof_ref[...], block, preferred_element_type=f32
        ).astype(bf16)


def run_expert(rows, gate, up, down):
    height, quarter = rows.shape
    steps = 4
    block = height // steps
    size = CELLS * TILE
    fixed = lambda i: (0, 0)
    return pl.pallas_call(
        expert_kernel,
        grid=(steps,),
        in_specs=[
            pl.BlockSpec((block, quarter), lambda i: (i, 0)),
            pl.BlockSpec(gate.shape, fixed),
            pl.BlockSpec(up.shape, fixed),
            pl.BlockSpec(down.shape, fixed),
            pl.BlockSpec((size, size), fixed),
            pl.BlockSpec((size, size), fixed),
        ],
        out_specs=pl.BlockSpec((block, quarter), lambda i: (i, 0)),
        out_shape=jax.ShapeDtypeStruct(rows.shape, rows.dtype),
        compiler_params=pltpu.CompilerParams(
            dimension_semantics=("arbitrary",), vmem_limit_bytes=48 * 1024 * 1024
        ),
        name="expert",
    )(rows, gate, up, down, reorder(CELLS, False), reorder(CELLS, True))


def body(
    mixer_in,
    mixer_gain,
    w_query,
    w_key,
    w_value,
    sink_logit,
    moe_in,
    moe_gain,
    router,
    routes,
    expert_gate,
    expert_up,
    expert_down,
    shared_gate,
    shared_up,
    shared_down,
):
    f32, bf16 = jnp.float32, jnp.bfloat16
    columns, rows = lax.axis_size("tp"), lax.axis_size("ep")
    normed_first = rms_rows(mixer_in, mixer_gain)
    normed_second = rms_rows(moe_in, moe_gain)
    tokens, width = normed_second.shape
    experts = router.shape[1]
    quarter = width // FOLD

    named = routes.T
    hit = jnp.any(named[None] == jnp.arange(experts, dtype=jnp.int32)[:, None, None], axis=1)
    earlier = (jnp.arange(tokens)[:, None] < jnp.arange(tokens)[None, :]).astype(bf16)
    rank = jnp.dot(hit.astype(bf16), earlier, preferred_element_type=f32)
    code = jnp.where(hit, rank, -1.0)
    place = jnp.arange(TILE, dtype=jnp.int32)
    lane = jnp.arange(FOLD * tokens, dtype=jnp.int32)
    same_fold = (place[:, None] // CAP) == (lane[None, :] // tokens)
    picks = (jnp.tile(code, (1, FOLD))[:, None, :] == (place % CAP).astype(f32)[None, :, None]) & same_fold[None]
    stacked_rows = jnp.concatenate(
        [normed_second[:, f * quarter : (f + 1) * quarter] for f in range(FOLD)], axis=0
    )
    outgoing = jnp.dot(
        picks.astype(bf16).reshape(experts * TILE, FOLD * tokens),
        stacked_rows,
        preferred_element_type=f32,
    ).astype(bf16)
    arrived = lax.all_to_all(
        outgoing.reshape(experts, TILE, quarter), ("ep", "tp"), split_axis=0, concat_axis=0, tiled=True
    )
    results = run_expert(
        arrived.reshape(experts * TILE, quarter), expert_gate[0], expert_up[0], expert_down[0]
    )
    returned = lax.all_to_all(
        results.reshape(experts, TILE, quarter), ("ep", "tp"), split_axis=0, concat_axis=0, tiled=True
    ).reshape(experts * TILE, quarter)

    affinity = jax.nn.sigmoid(
        lax.dot_general(router, normed_second, (((0,), (1,)), ((), ())), preferred_element_type=f32)
    )
    chosen = jnp.where(hit, affinity, 0.0)
    weight = ROUTED_SCALE * chosen / jnp.sum(chosen, axis=0, keepdims=True)
    coarse = lax.reduce_precision(weight, 8, 7)

    def mixing(scale):
        spread = jnp.tile(scale.astype(bf16), (1, FOLD))[:, None, :]
        return jnp.where(picks, spread, 0.0).reshape(experts * TILE, FOLD * tokens)

    def mixed_by(scale):
        return lax.dot_general(
            mixing(scale), returned, (((0,), (0,)), ((), ())), preferred_element_type=f32
        )

    routed = mixed_by(coarse) + mixed_by(weight - coarse)
    routed = jnp.concatenate([routed[f * tokens : (f + 1) * tokens] for f in range(FOLD)], axis=1)

    part = width // rows
    start = lax.axis_index("ep") * part
    piece = jnp.concatenate(
        [
            lax.dynamic_slice_in_dim(jnp.concatenate([shared_gate, shared_up], axis=1), start, part, 0),
            lax.dynamic_slice_in_dim(shared_down, start, part, 1),
        ],
        axis=0,
    )
    units = shared_gate.shape[1]
    whole = lax.all_gather(piece, ("ep", "tp"), axis=0, tiled=False)
    whole = whole.reshape(rows, columns, part + units, part)
    both = jnp.transpose(whole[:, :, :part], (0, 2, 1, 3)).reshape(width, columns * 2 * units)
    full_down = jnp.transpose(whole[:, :, part:], (1, 2, 0, 3)).reshape(columns * units, width)
    lifted = jnp.dot(normed_second, both, preferred_element_type=f32).reshape(tokens, columns, 2 * units)
    hidden = (jax.nn.silu(lifted[..., :units]) * lifted[..., units:]).astype(bf16)
    shared = jnp.dot(hidden.reshape(tokens, columns * units), full_down, preferred_element_type=f32)
    moe_out = (routed + shared).astype(bf16)

    query_cols = w_query.shape[1]
    key_cols = w_key.shape[1]
    joined = jnp.concatenate([w_query, w_key, w_value], axis=1)
    projected = jnp.dot(
        lax.all_gather(normed_first, "tp", axis=0, tiled=True),
        joined,
        preferred_element_type=jnp.float32,
    )
    span_rows = projected.shape[0]
    offset = lax.axis_index("ep") * span_rows
    seq_length = span_rows * lax.axis_size("ep")
    positions = offset + jnp.arange(span_rows, dtype=jnp.int32)
    query_rows = rotate(
        projected[:, :query_cols].reshape(span_rows, -1, HEAD_DIM), positions
    ).astype(jnp.bfloat16)
    key_rows = rotate(
        projected[:, query_cols : query_cols + key_cols].reshape(span_rows, -1, HEAD_DIM), positions
    ).astype(jnp.bfloat16)
    value_rows = projected[:, query_cols + key_cols :].astype(jnp.bfloat16)
    stacked = jnp.concatenate([key_rows.reshape(span_rows, key_cols), value_rows], axis=1)
    padded = extended(stacked, (("ep", 0),), WINDOW)
    mixed = attend(query_rows, padded, sink_logit, offset, seq_length)
    return (mixed, moe_out)


def solution(mesh):
    return jax.shard_map(
        body,
        mesh=mesh,
        in_specs=(
            P(("grp", "ep", "tp"), None),
            P(),
            P(None, "tp"),
            P(None, "tp"),
            P(None, "tp"),
            P("tp"),
            P(("grp", "ep", "tp"), None),
            P(),
            P(),
            P(("grp", "ep", "tp"), None),
            P(("ep", "tp"), None, None),
            P(("ep", "tp"), None, None),
            P(("ep", "tp"), None, None),
            P(None, "tp"),
            P(None, "tp"),
            P("tp", None),
        ),
        out_specs=(P(("grp", "ep"), "tp"), P(("grp", "ep", "tp"), None)),
        check_vma=False,
    )
```

```python
import jax
import jax.numpy as jnp
from jax import lax
from jax.experimental import pallas as pl
from jax.experimental.pallas import tpu as pltpu
from jax.sharding import PartitionSpec as P

HEAD_DIM = 64
WINDOW = 128


EPS = 1e-06
THETA = 10000.0
ROUTED_SCALE = 2.5


def extended(block, sides, width):
    for axis, dim in sides:
        count = lax.axis_size(axis)
        forward = [(i, i + 1) for i in range(count - 1)]
        backward = [(target, source) for source, target in forward]
        low = lax.ppermute(
            lax.slice_in_dim(block, block.shape[dim] - width, None, axis=dim), axis, forward
        )
        high = lax.ppermute(lax.slice_in_dim(block, 0, width, axis=dim), axis, backward)
        block = jnp.concatenate([low, block, high], axis=dim)
    return block


def rms_rows(row_block, gain_vector):
    values = row_block.astype(jnp.float32)
    factor = lax.rsqrt(jnp.mean(values * values, axis=-1, keepdims=True) + EPS)
    return (values * factor * gain_vector).astype(jnp.bfloat16)


def rotate(head_rows, positions):
    half_width = head_rows.shape[-1] // 2
    inverse = THETA ** (-(jnp.arange(half_width, dtype=jnp.float32) * 2.0) / head_rows.shape[-1])
    angles = positions.astype(jnp.float32)[:, None] * inverse[None, :]
    cosine_table = jnp.cos(angles)[:, None, :]
    sine_table = jnp.sin(angles)[:, None, :]
    first_half = head_rows[..., :half_width]
    second_half = head_rows[..., half_width:]
    return jnp.concatenate(
        [
            first_half * cosine_table - second_half * sine_table,
            second_half * cosine_table + first_half * sine_table,
        ],
        axis=-1,
    )


def attend(query_rows, stacked, sink_logit, offset, seq_length):
    span_rows, head_count, head_width = query_rows.shape
    kv_local = stacked.shape[1] // (2 * head_width)
    group_size = head_count // kv_local
    key_table = stacked[:, : kv_local * head_width].reshape(-1, kv_local, head_width)
    value_table = stacked[:, kv_local * head_width :].reshape(-1, kv_local, head_width)
    block_rows = 512
    grouped = query_rows.reshape(span_rows, kv_local, group_size, head_width)
    row_ids = jnp.arange(block_rows, dtype=jnp.int32)[:, None]
    col_ids = jnp.arange(block_rows + 2 * WINDOW, dtype=jnp.int32)[None, :]
    sink_table = sink_logit.reshape(kv_local, group_size)[:, :, None, None]

    def one_block(block_index):
        block_start = block_index * block_rows
        query_block = lax.dynamic_slice_in_dim(grouped, block_start, block_rows, 0)
        key_block = lax.dynamic_slice_in_dim(key_table, block_start, block_rows + 2 * WINDOW, 0)
        value_block = lax.dynamic_slice_in_dim(value_table, block_start, block_rows + 2 * WINDOW, 0)
        scores = jnp.einsum(
            "qkgd,ckd->kgqc", query_block, key_block, preferred_element_type=jnp.float32
        ) * head_width ** (-0.5)
        key_pos = offset + block_start - WINDOW + col_ids
        query_pos = offset + block_start + row_ids
        in_window = (
            (jnp.abs(key_pos - query_pos) <= WINDOW) & (key_pos >= 0) & (key_pos < seq_length)
        )
        scores = jnp.where(in_window[None, None], scores, -jnp.inf)
        row_max = jnp.maximum(jnp.max(scores, axis=-1, keepdims=True), sink_table)
        weights = jnp.exp(scores - row_max)
        denominator = jnp.sum(weights, axis=-1, keepdims=True) + jnp.exp(sink_table - row_max)
        probability = (weights / denominator).astype(jnp.bfloat16)
        output = jnp.einsum(
            "kgqc,ckd->qkgd", probability, value_block, preferred_element_type=jnp.float32
        )
        return output.reshape(block_rows, head_count * head_width).astype(jnp.bfloat16)

    blocks_out = lax.map(one_block, jnp.arange(span_rows // block_rows, dtype=jnp.int32))
    return blocks_out.reshape(span_rows, head_count * head_width)


CAP = 6
CHUNKS = ((0, 1, -1, 2), (-2, 3, -3, 4))


def ring(count, step):
    return [(i, (i + step) % count) for i in range(count)]


def ring_gather(block, axis, keep):
    count = lax.axis_size(axis)
    blocks, ahead, behind = {0: block}, block, block
    for step in range(1, (count + 1) // 2):
        behind = lax.ppermute(behind, axis, ring(count, 1))
        ahead = lax.ppermute(ahead, axis, ring(count, -1))
        blocks[-step], blocks[step] = behind, ahead
    half = block.shape[1] // 2
    low = lax.ppermute(behind[:, :half], axis, ring(count, 1))
    high = lax.ppermute(ahead[:, half:], axis, ring(count, -1))
    blocks[count // 2] = jnp.concatenate([low, high], axis=1)
    return blocks


def ring_scatter(parts, axis):
    count = lax.axis_size(axis)
    f32, bf16 = jnp.float32, jnp.bfloat16
    far = parts[count // 2].astype(bf16)
    half = far.shape[1] // 2
    forth = lax.ppermute(far[:, :half], axis, ring(count, 1))
    back = lax.ppermute(far[:, half:], axis, ring(count, -1))
    zeros = jnp.zeros_like(forth)
    forth = jnp.concatenate([forth, zeros], axis=1)
    back = jnp.concatenate([zeros, back], axis=1)
    for step in range((count - 1) // 2, 0, -1):
        one = (parts[step] + forth.astype(f32)).astype(bf16)
        two = (parts[-step] + back.astype(f32)).astype(bf16)
        forth = lax.ppermute(one, axis, ring(count, 1))
        back = lax.ppermute(two, axis, ring(count, -1))
    return parts[0] + forth.astype(f32) + back.astype(f32)


def slot_tables(here_ref, height, members, columns):
    row = lax.broadcasted_iota(jnp.int32, (height, 128), 0)
    per = height // members
    member = sum([(row >= m * per).astype(jnp.int32) for m in range(1, members)])
    within = row - member * per
    block = sum([(within >= b * CAP).astype(jnp.int32) for b in range(1, per // CAP)])
    slot = within - block * CAP
    expert = member * columns + here_ref[0]
    return expert.astype(jnp.float32), block, slot.astype(jnp.float32)


def picked(routes, expert, mine, slot, earlier):
    hit = routes[0:1] == expert
    for k in range(1, 4):
        hit = hit | (routes[k : k + 1] == expert)
    hit = hit & mine
    rank = jnp.dot(hit.astype(jnp.bfloat16), earlier, preferred_element_type=jnp.float32)
    return hit & (rank == slot)


def before(tokens):
    return (
        lax.broadcasted_iota(jnp.int32, (tokens, tokens), 0)
        < lax.broadcasted_iota(jnp.int32, (tokens, tokens), 1)
    ).astype(jnp.bfloat16)


def pack_kernel(members, columns, tokens, here_ref, *refs):
    out_ref = refs[-1]
    expert, block, slot = slot_tables(here_ref, out_ref.shape[0], members, columns)
    earlier = before(tokens)
    picks, sources = [], []
    for place, ref in enumerate(refs[:-1]):
        routes = ref[tokens:, :tokens].astype(jnp.float32)
        picks.append(picked(routes, expert, block == place, slot, earlier).astype(jnp.bfloat16))
        sources.append(ref[:tokens])
    out_ref[...] = jnp.dot(
        jnp.concatenate(picks, axis=1),
        jnp.concatenate(sources, axis=0),
        preferred_element_type=jnp.float32,
    ).astype(jnp.bfloat16)


def mix_kernel(members, columns, tokens, here_ref, *refs):
    back_ref, router_ref, gate_ref, up_ref, down_ref, out_ref = refs[-6:]
    f32, bf16 = jnp.float32, jnp.bfloat16
    height = back_ref.shape[0]
    expert, block, slot = slot_tables(here_ref, height, members, columns)
    experts = router_ref.shape[0]
    earlier = before(tokens)
    number = lax.broadcasted_iota(jnp.int32, (experts, tokens), 0).astype(f32)
    wanted = (lax.broadcasted_iota(jnp.int32, (height, experts), 1).astype(f32) == expert).astype(bf16)
    coarse, fine, sources = [], [], []
    for place, ref in enumerate(refs[:-6]):
        routes = ref[tokens:, :tokens].astype(f32)
        source = ref[:tokens]
        logits = lax.dot_general(
            router_ref[...], source, (((1,), (1,)), ((), ())), preferred_element_type=f32
        )
        affinity = 1.0 / (1.0 + jnp.exp(-logits))
        named = routes[0:1] == number
        for k in range(1, 4):
            named = named | (routes[k : k + 1] == number)
        chosen = jnp.where(named, affinity, 0.0)
        weight = ROUTED_SCALE * chosen / jnp.sum(chosen, axis=0, keepdims=True)
        high = weight.astype(bf16)
        low = (weight - high.astype(f32)).astype(bf16)
        pick = picked(routes, expert, block == place, slot, earlier)
        coarse.append(
            jnp.where(pick, jnp.dot(wanted, high, preferred_element_type=f32), 0.0).astype(bf16)
        )
        fine.append(
            jnp.where(pick, jnp.dot(wanted, low, preferred_element_type=f32), 0.0).astype(bf16)
        )
        sources.append(source)
    rows = jnp.concatenate(sources, axis=0)
    gate = jnp.dot(rows, gate_ref[...], preferred_element_type=f32)
    up = jnp.dot(rows, up_ref[...], preferred_element_type=f32)
    hidden = (gate * (1.0 / (1.0 + jnp.exp(-gate))) * up).astype(bf16)
    over = (((0,), (0,)), ((), ()))
    out_ref[...] = (
        lax.dot_general(jnp.concatenate(coarse, axis=1), back_ref[...], over, preferred_element_type=f32)
        + lax.dot_general(jnp.concatenate(fine, axis=1), back_ref[...], over, preferred_element_type=f32)
        + jnp.dot(hidden, down_ref[...], preferred_element_type=f32)
    )


def local_call(kernel, here, arrays, shape, dtype, name, flops):
    whole = pl.BlockSpec(memory_space=pltpu.VMEM)
    return pl.pallas_call(
        kernel,
        in_specs=[pl.BlockSpec(memory_space=pltpu.SMEM)] + [whole] * len(arrays),
        out_specs=whole,
        out_shape=jax.ShapeDtypeStruct(shape, dtype),
        compiler_params=pltpu.CompilerParams(vmem_limit_bytes=48 * 1024 * 1024),
        cost_estimate=pl.CostEstimate(flops=flops, bytes_accessed=1 << 23, transcendentals=0),
        name=name,
    )(here, *arrays)


def body(
    mixer_in,
    mixer_gain,
    w_query,
    w_key,
    w_value,
    sink_logit,
    moe_in,
    moe_gain,
    router,
    routes,
    expert_gate,
    expert_up,
    expert_down,
    shared_gate,
    shared_up,
    shared_down,
):
    f32, bf16 = jnp.float32, jnp.bfloat16
    columns, rows = lax.axis_size("tp"), lax.axis_size("ep")
    here = lax.axis_index("tp").astype(jnp.int32).reshape(1)
    tokens, width = moe_in.shape
    choices = routes.shape[1]
    listed = jnp.pad(routes.T.astype(bf16), ((0, 8 - choices), (0, width - tokens)))
    normed_second = jnp.concatenate([rms_rows(moe_in, moe_gain), listed], axis=0)
    blocks = ring_gather(normed_second, "tp", None)

    def exchange(rows_out):
        return lax.all_to_all(
            rows_out.reshape(rows, -1, width), "ep", split_axis=0, concat_axis=0, tiled=True
        ).reshape(rows_out.shape)

    def run_experts(flat_rows):
        hidden = (
            jax.nn.silu(jnp.dot(flat_rows, expert_gate[0], preferred_element_type=f32))
            * jnp.dot(flat_rows, expert_up[0], preferred_element_type=f32)
        ).astype(bf16)
        return jnp.dot(hidden, expert_down[0], preferred_element_type=f32).astype(bf16)

    turned_router = router.T
    arrived = []
    for chunk in CHUNKS:
        height = rows * len(chunk) * CAP
        sent = local_call(
            lambda *refs: pack_kernel(rows, columns, tokens, *refs),
            here,
            [blocks[d] for d in chunk],
            (height, width),
            bf16,
            "pack",
            2 * height * len(chunk) * tokens * width,
        )
        arrived.append(exchange(sent))
    parts = {}
    for chunk, got in list(zip(CHUNKS, arrived))[::-1]:
        back = exchange(run_experts(got))
        mixed_rows = local_call(
            lambda *refs: mix_kernel(rows, columns, tokens, *refs),
            here,
            [blocks[d] for d in chunk]
            + [back, turned_router, shared_gate, shared_up, shared_down],
            (len(chunk) * tokens, width),
            f32,
            "mix",
            4 * back.shape[0] * len(chunk) * tokens * width,
        )
        for place, d in enumerate(chunk):
            parts[d] = mixed_rows[place * tokens : (place + 1) * tokens]
    moe_out = ring_scatter(parts, "tp").astype(bf16)

    late = blocks[columns // 2][:1, :1] * 0.0
    normed_first = rms_rows(mixer_in + late, mixer_gain)
    query_cols = w_query.shape[1]
    key_cols = w_key.shape[1]
    joined = jnp.concatenate([w_query, w_key, w_value], axis=1)
    projected = jnp.dot(
        lax.all_gather(normed_first, "tp", axis=0, tiled=True),
        joined,
        preferred_element_type=jnp.float32,
    )
    span_rows = projected.shape[0]
    offset = lax.axis_index("ep") * span_rows
    seq_length = span_rows * lax.axis_size("ep")
    positions = offset + jnp.arange(span_rows, dtype=jnp.int32)
    query_rows = rotate(
        projected[:, :query_cols].reshape(span_rows, -1, HEAD_DIM), positions
    ).astype(jnp.bfloat16)
    key_rows = rotate(
        projected[:, query_cols : query_cols + key_cols].reshape(span_rows, -1, HEAD_DIM), positions
    ).astype(jnp.bfloat16)
    value_rows = projected[:, query_cols + key_cols :].astype(jnp.bfloat16)
    stacked = jnp.concatenate([key_rows.reshape(span_rows, key_cols), value_rows], axis=1)
    padded = extended(stacked, (("ep", 0),), WINDOW)
    mixed = attend(query_rows, padded, sink_logit, offset, seq_length)
    return (mixed, moe_out)


def solution(mesh):
    return jax.shard_map(
        body,
        mesh=mesh,
        in_specs=(
            P(("grp", "ep", "tp"), None),
            P(),
            P(None, "tp"),
            P(None, "tp"),
            P(None, "tp"),
            P("tp"),
            P(("grp", "ep", "tp"), None),
            P(),
            P(),
            P(("grp", "ep", "tp"), None),
            P(("ep", "tp"), None, None),
            P(("ep", "tp"), None, None),
            P(("ep", "tp"), None, None),
            P(None, "tp"),
            P(None, "tp"),
            P("tp", None),
        ),
        out_specs=(P(("grp", "ep"), "tp"), P(("grp", "ep", "tp"), None)),
        check_vma=False,
    )
```

```python
import jax
import jax.numpy as jnp
from jax import lax
from jax.experimental import pallas as pl
from jax.experimental.pallas import tpu as pltpu
from jax.sharding import PartitionSpec as P

HEAD_DIM = 64
WINDOW = 128


EPS = 1e-06
THETA = 10000.0
ROUTED_SCALE = 2.5


def extended(block, sides, width):
    for axis, dim in sides:
        count = lax.axis_size(axis)
        forward = [(i, i + 1) for i in range(count - 1)]
        backward = [(target, source) for source, target in forward]
        low = lax.ppermute(
            lax.slice_in_dim(block, block.shape[dim] - width, None, axis=dim), axis, forward
        )
        high = lax.ppermute(lax.slice_in_dim(block, 0, width, axis=dim), axis, backward)
        block = jnp.concatenate([low, block, high], axis=dim)
    return block


def rms_rows(row_block, gain_vector):
    values = row_block.astype(jnp.float32)
    factor = lax.rsqrt(jnp.mean(values * values, axis=-1, keepdims=True) + EPS)
    return (values * factor * gain_vector).astype(jnp.bfloat16)


def attend(query_rows, stacked, sink_logit, offset, seq_length):
    span_rows, head_count, head_width = query_rows.shape
    kv_local = stacked.shape[1] // (2 * head_width)
    group_size = head_count // kv_local
    key_table = stacked[:, : kv_local * head_width].reshape(-1, kv_local, head_width)
    value_table = stacked[:, kv_local * head_width :].reshape(-1, kv_local, head_width)
    block_rows = 512
    grouped = query_rows.reshape(span_rows, kv_local, group_size, head_width)
    row_ids = jnp.arange(block_rows, dtype=jnp.int32)[:, None]
    col_ids = jnp.arange(block_rows + 2 * WINDOW, dtype=jnp.int32)[None, :]
    sink_table = sink_logit.reshape(kv_local, group_size)[:, :, None, None]

    def one_block(block_index):
        block_start = block_index * block_rows
        query_block = lax.dynamic_slice_in_dim(grouped, block_start, block_rows, 0)
        key_block = lax.dynamic_slice_in_dim(key_table, block_start, block_rows + 2 * WINDOW, 0)
        value_block = lax.dynamic_slice_in_dim(value_table, block_start, block_rows + 2 * WINDOW, 0)
        scores = jnp.einsum(
            "qkgd,ckd->kgqc", query_block, key_block, preferred_element_type=jnp.float32
        ) * head_width ** (-0.5)
        key_pos = offset + block_start - WINDOW + col_ids
        query_pos = offset + block_start + row_ids
        in_window = (
            (jnp.abs(key_pos - query_pos) <= WINDOW) & (key_pos >= 0) & (key_pos < seq_length)
        )
        scores = jnp.where(in_window[None, None], scores, -jnp.inf)
        row_max = jnp.maximum(jnp.max(scores, axis=-1, keepdims=True), sink_table)
        weights = jnp.exp(scores - row_max)
        denominator = jnp.sum(weights, axis=-1, keepdims=True) + jnp.exp(sink_table - row_max)
        probability = (weights / denominator).astype(jnp.bfloat16)
        output = jnp.einsum(
            "kgqc,ckd->qkgd", probability, value_block, preferred_element_type=jnp.float32
        )
        return output.reshape(block_rows, head_count * head_width).astype(jnp.bfloat16)

    blocks_out = lax.map(one_block, jnp.arange(span_rows // block_rows, dtype=jnp.int32))
    return blocks_out.reshape(span_rows, head_count * head_width)


CAP = 6
CHUNKS = ((0, 1, -1, 2), (-2, 3, -3, 4))
F32, BF16 = jnp.float32, jnp.bfloat16


def ring(count, step):
    return [(i, (i + step) % count) for i in range(count)]


def ring_gather(block, axis):
    count = lax.axis_size(axis)
    blocks, ahead, behind = {0: block}, block, block
    for step in range(1, (count + 1) // 2):
        behind = lax.ppermute(behind, axis, ring(count, 1))
        ahead = lax.ppermute(ahead, axis, ring(count, -1))
        blocks[-step], blocks[step] = behind, ahead
    half, step = block.shape[1] // 2, count // 2
    low = lax.ppermute(behind[:, :half], axis, ring(count, 1))
    high = lax.ppermute(ahead[:, half:], axis, ring(count, -1))
    blocks[step] = jnp.concatenate([low, high], axis=1)
    return blocks


def ring_scatter(parts, far, axis):
    count = lax.axis_size(axis)
    forth = lax.ppermute(far[0], axis, ring(count, 1))
    back = lax.ppermute(far[1], axis, ring(count, -1))
    zeros = jnp.zeros_like(forth)
    forth = jnp.concatenate([forth, zeros], axis=1)
    back = jnp.concatenate([zeros, back], axis=1)
    for step in range((count - 1) // 2, 0, -1):
        one = (parts[step] + forth.astype(F32)).astype(BF16)
        two = (parts[-step] + back.astype(F32)).astype(BF16)
        forth = lax.ppermute(one, axis, ring(count, 1))
        back = lax.ppermute(two, axis, ring(count, -1))
    return (parts[0] + forth.astype(F32) + back.astype(F32)).astype(BF16)


def slot_tables(here_ref, height, members, columns):
    row = lax.broadcasted_iota(jnp.int32, (height, 128), 0)
    per = height // members
    member = sum([(row >= m * per).astype(jnp.int32) for m in range(1, members)])
    within = row - member * per
    block = sum([(within >= b * CAP).astype(jnp.int32) for b in range(1, per // CAP)])
    slot = within - block * CAP
    expert = member * columns + here_ref[0]
    return expert.astype(F32), block, slot.astype(F32)


def names(routes, number):
    hit = routes[0:1] == number
    for k in range(1, 4):
        hit = hit | (routes[k : k + 1] == number)
    return hit


def picked(routes, expert, mine, slot, earlier):
    hit = names(routes, expert) & mine
    rank = jnp.dot(hit.astype(BF16), earlier, preferred_element_type=F32)
    return hit & (rank == slot)


def before(tokens):
    return (
        lax.broadcasted_iota(jnp.int32, (tokens, tokens), 0)
        < lax.broadcasted_iota(jnp.int32, (tokens, tokens), 1)
    ).astype(BF16)


def silu(v):
    return v * (1.0 / (1.0 + jnp.exp(-v)))


def pack_kernel(members, columns, tokens, here_ref, *refs):
    out_ref = refs[-1]
    expert, block, slot = slot_tables(here_ref, out_ref.shape[0], members, columns)
    earlier = before(tokens)
    picks, sources = [], []
    for place, ref in enumerate(refs[:-1]):
        routes = ref[tokens:, :tokens].astype(F32)
        picks.append(picked(routes, expert, block == place, slot, earlier).astype(BF16))
        sources.append(ref[:tokens])
    out_ref[...] = jnp.dot(
        jnp.concatenate(picks, axis=1),
        jnp.concatenate(sources, axis=0),
        preferred_element_type=F32,
    ).astype(BF16)


def prepare_kernel(members, columns, tokens, height, here_ref, *refs):
    router_ref, gate_ref, up_ref, coarse_ref, fine_ref, hidden_ref = refs[-6:]
    expert, block, slot = slot_tables(here_ref, height, members, columns)
    experts = router_ref.shape[1]
    earlier = before(tokens)
    number = lax.broadcasted_iota(jnp.int32, (experts, tokens), 0).astype(F32)
    wanted = (lax.broadcasted_iota(jnp.int32, (height, experts), 1).astype(F32) == expert).astype(BF16)
    across = (((1,), (1,)), ((), ()))
    for place, ref in enumerate(refs[:-6]):
        routes = ref[tokens:, :tokens].astype(F32)
        source = ref[:tokens]
        logits = jnp.dot(source, router_ref[...], preferred_element_type=F32).T
        affinity = 1.0 / (1.0 + jnp.exp(-logits))
        chosen = jnp.where(names(routes, number), affinity, 0.0)
        weight = ROUTED_SCALE * chosen / jnp.sum(chosen, axis=0, keepdims=True)
        high = weight.astype(BF16)
        low = (weight - high.astype(F32)).astype(BF16)
        pick = picked(routes, expert, block == place, slot, earlier)
        span = slice(place * tokens, (place + 1) * tokens)
        for part, out in ((high, coarse_ref), (low, fine_ref)):
            spread = jnp.where(pick, jnp.dot(wanted, part, preferred_element_type=F32), 0.0)
            out[span] = spread.T.astype(BF16)
        gate = lax.dot_general(source, gate_ref[...], across, preferred_element_type=F32)
        up = lax.dot_general(source, up_ref[...], across, preferred_element_type=F32)
        hidden_ref[span] = (silu(gate) * up).astype(BF16)


def mix_kernel(tokens, coarse_ref, fine_ref, hidden_ref, back_ref, down_ref, *outs):
    total = (
        jnp.dot(coarse_ref[...], back_ref[...], preferred_element_type=F32)
        + jnp.dot(fine_ref[...], back_ref[...], preferred_element_type=F32)
        + jnp.dot(hidden_ref[...], down_ref[...], preferred_element_type=F32)
    )
    at = 0
    for out in outs:
        if out.dtype == F32:
            out[...] = total[at : at + tokens]
            at += tokens
        else:
            half = out.shape[1]
            start = 0 if out is outs[-2] else half
            out[...] = total[at : at + tokens, start : start + half].astype(BF16)


def local_call(kernel, here, arrays, shapes, flops):
    whole = pl.BlockSpec(memory_space=pltpu.VMEM)
    first = [] if here is None else [pl.BlockSpec(memory_space=pltpu.SMEM)]
    return pl.pallas_call(
        kernel,
        in_specs=first + [whole] * len(arrays),
        out_specs=[whole] * len(shapes),
        out_shape=shapes,
        compiler_params=pltpu.CompilerParams(vmem_limit_bytes=40 * 1024 * 1024),
        cost_estimate=pl.CostEstimate(flops=flops, bytes_accessed=1 << 23, transcendentals=0),
    )(*([] if here is None else [here]), *arrays)


def expert_kernel(rows_ref, gate_ref, up_ref, down_ref, *rest):
    out_ref, sum_ref = rest[-2:]
    step = pl.program_id(0)
    rows = rows_ref[...]
    gate = jnp.dot(rows, gate_ref[0], preferred_element_type=F32)
    up = jnp.dot(rows, up_ref[0], preferred_element_type=F32)
    hidden = (silu(gate) * up).astype(BF16)
    part = jnp.dot(hidden, down_ref[0], preferred_element_type=F32)

    @pl.when(step == 0)
    def _():
        sum_ref[...] = part

    @pl.when(step == pl.num_programs(0) - 1)
    def _():
        out_ref[...] = (sum_ref[...] + part).astype(BF16)


def run_experts(rows, gate, up, down, waits):
    height, width = rows.shape
    units = gate.shape[2]
    half = units // 2
    return pl.pallas_call(
        expert_kernel,
        grid=(2,),
        in_specs=[
            pl.BlockSpec((height, width), lambda i: (0, 0)),
            pl.BlockSpec((1, width, half), lambda i: (0, 0, i)),
            pl.BlockSpec((1, width, half), lambda i: (0, 0, i)),
            pl.BlockSpec((1, half, width), lambda i: (0, i, 0)),
        ]
        + [pl.BlockSpec(memory_space=pl.ANY)] * len(waits),
        out_specs=pl.BlockSpec((height, width), lambda i: (0, 0)),
        out_shape=jax.ShapeDtypeStruct(rows.shape, rows.dtype),
        scratch_shapes=[pltpu.VMEM((height, width), F32)],
        compiler_params=pltpu.CompilerParams(
            dimension_semantics=("arbitrary",), vmem_limit_bytes=40 * 1024 * 1024
        ),
        cost_estimate=pl.CostEstimate(
            flops=6 * height * width * units, bytes_accessed=3 * 2 * width * units, transcendentals=0
        ),
        name="expert",
    )(rows, gate, up, down, *waits)


def project_kernel(columns, tokens, here_ref, *refs):
    query_w, key_w, value_w, cos_ref, sin_ref, query_ref, stacked_ref = refs[-7:]
    across = (((1,), (1,)), ((), ()))
    lane = lax.broadcasted_iota(jnp.int32, (tokens, query_ref.shape[1]), 1)
    first = (lane % HEAD_DIM) < HEAD_DIM // 2

    def turned(values, cosine, sine):
        other = jnp.where(
            first,
            pltpu.roll(values, values.shape[1] - HEAD_DIM // 2, 1),
            pltpu.roll(values, HEAD_DIM // 2, 1),
        )
        return (values * cosine + other * sine).astype(BF16)

    keyed = lane < HEAD_DIM
    for distance, ref in enumerate(refs[:-7]):
        spot = lax.rem(here_ref[0] + distance, columns) * tokens
        span = pl.ds(pl.multiple_of(spot, tokens), tokens)
        rows = ref[...]
        query = jnp.dot(rows, query_w[...], preferred_element_type=F32)
        pair = jnp.concatenate(
            [
                lax.dot_general(rows, key_w[...], across, preferred_element_type=F32),
                lax.dot_general(rows, value_w[...], across, preferred_element_type=F32),
            ],
            axis=1,
        )
        cosine, sine = cos_ref[span], sin_ref[span]
        cosine = jnp.concatenate([cosine] * 4, axis=1)
        sine = jnp.concatenate([-sine, sine] * 2, axis=1)
        query_ref[span] = turned(query, cosine, sine)
        stacked_ref[span] = turned(
            pair, jnp.where(keyed, cosine, 1.0), jnp.where(keyed, sine, 0.0)
        )


def body(
    mixer_in,
    mixer_gain,
    w_query,
    w_key,
    w_value,
    sink_logit,
    moe_in,
    moe_gain,
    router,
    routes,
    expert_gate,
    expert_up,
    expert_down,
    shared_gate,
    shared_up,
    shared_down,
):
    columns, rows = lax.axis_size("tp"), lax.axis_size("ep")
    here = lax.axis_index("tp").astype(jnp.int32).reshape(1)
    tokens, width = moe_in.shape
    listed = jnp.pad(routes.T.astype(BF16), ((0, 8 - routes.shape[1]), (0, width - tokens)))
    normed_second = jnp.concatenate([rms_rows(moe_in, moe_gain), listed], axis=0)
    blocks = ring_gather(normed_second, "tp")

    def exchange(rows_out):
        return lax.all_to_all(
            rows_out.reshape(rows, -1, width), "ep", split_axis=0, concat_axis=0, tiled=True
        ).reshape(rows_out.shape)

    late = blocks[columns // 2][:1, :1] * 0.0
    normed_first = rms_rows(mixer_in + late, mixer_gain)
    mixer_blocks = ring_gather(normed_first, "tp")
    span_rows = tokens * columns
    offset = lax.axis_index("ep") * span_rows
    seq_length = span_rows * rows
    positions = (offset + jnp.arange(span_rows, dtype=jnp.int32)).astype(F32)
    half_width = HEAD_DIM // 2
    inverse = THETA ** (-(jnp.arange(half_width, dtype=F32) * 2.0) / HEAD_DIM)
    angles = positions[:, None] * inverse[None, :]
    heads = w_query.shape[1] // HEAD_DIM
    query_rows, stacked = local_call(
        lambda *refs: project_kernel(columns, tokens, *refs),
        here,
        [mixer_blocks[d if d <= columns // 2 else d - columns] for d in range(columns)]
        + [
            w_query,
            w_key.T,
            w_value.T,
            jnp.cos(angles),
            jnp.sin(angles),
        ],
        [
            jax.ShapeDtypeStruct((span_rows, w_query.shape[1]), BF16),
            jax.ShapeDtypeStruct((span_rows, w_key.shape[1] + w_value.shape[1]), BF16),
        ],
        2 * span_rows * width * 2 * w_query.shape[1],
    )
    padded = extended(stacked, (("ep", 0),), WINDOW)
    mixed = attend(
        query_rows.reshape(span_rows, heads, HEAD_DIM), padded, sink_logit, offset, seq_length
    )

    arrived, ready = [], []
    for chunk in CHUNKS:
        height = rows * len(chunk) * CAP
        used = [blocks[d] for d in chunk]
        sent = local_call(
            lambda *refs: pack_kernel(rows, columns, tokens, *refs),
            here,
            used,
            [jax.ShapeDtypeStruct((height, width), BF16)],
            2 * height * len(chunk) * tokens * width,
        )[0]
        arrived.append(exchange(sent))
        stacked_rows = len(chunk) * tokens
        ready.append(
            local_call(
                lambda *refs: prepare_kernel(rows, columns, tokens, height, *refs),
                here,
                used + [router, shared_gate.T, shared_up.T],
                [
                    jax.ShapeDtypeStruct((stacked_rows, height), BF16),
                    jax.ShapeDtypeStruct((stacked_rows, height), BF16),
                    jax.ShapeDtypeStruct((stacked_rows, shared_gate.shape[1]), BF16),
                ],
                8 * stacked_rows * width * router.shape[1],
            )
        )
    parts, far = {}, None
    waits = ([mixed] + [made[0] for made in ready], [])
    for number in reversed(range(len(CHUNKS))):
        chunk = CHUNKS[number]
        results = run_experts(
            arrived[number], expert_gate, expert_up, expert_down, waits[number]
        )
        back = exchange(results)
        plain = [d for d in chunk if d != columns // 2]
        outs = [jax.ShapeDtypeStruct((tokens, width), F32)] * len(plain)
        if len(plain) < len(chunk):
            outs = outs + [jax.ShapeDtypeStruct((tokens, width // 2), BF16)] * 2
        made = local_call(
            lambda *refs: mix_kernel(tokens, *refs),
            None,
            list(ready[number]) + [back, shared_down],
            outs,
            4 * back.shape[0] * len(chunk) * tokens * width,
        )
        for d, value in zip(plain, made):
            parts[d] = value
        if len(plain) < len(chunk):
            far = made[-2:]
    moe_out = ring_scatter(parts, far, "tp")
    return (mixed, moe_out)


def solution(mesh):
    return jax.shard_map(
        body,
        mesh=mesh,
        in_specs=(
            P(("grp", "ep", "tp"), None),
            P(),
            P(None, "tp"),
            P(None, "tp"),
            P(None, "tp"),
            P("tp"),
            P(("grp", "ep", "tp"), None),
            P(),
            P(),
            P(("grp", "ep", "tp"), None),
            P(("ep", "tp"), None, None),
            P(("ep", "tp"), None, None),
            P(("ep", "tp"), None, None),
            P(None, "tp"),
            P(None, "tp"),
            P("tp", None),
        ),
        out_specs=(P(("grp", "ep"), "tp"), P(("grp", "ep", "tp"), None)),
        check_vma=False,
    )
```
